32 devices in a mesh: grp: 2 (over y), sp: 4 (over z), tp: 4 (over x, core).
Axes of the slice: x: 2, y: 2, z: 4, core: 2. Of those that a mesh axis runs over, the one named last changes fastest.
Arguments:
- queries: bfloat16 [4096, 2048], P(('grp', 'sp'), 'tp'), parts along dimension 0, may hold values from -64 to 64
- key_heads: bfloat16 [4096, 4, 64], P(('grp', 'sp'), 'tp'), parts along dimension 0, may hold values from -64 to 64
- value_heads: bfloat16 [4096, 4, 64], P(('grp', 'sp'), 'tp'), parts along dimension 0, may hold values from -6 to 6
- sink_logit: float32 [32], P('tp'), may hold values from 3 to 6
- out_weight: bfloat16 [2048, 2048], P('tp'), may hold values from -0.75 to 0.75
- residual: bfloat16 [4096, 2048], P(('grp', 'sp', 'tp')), parts along dimension 0, may hold values from -6 to 6
- norm_gain: float32 [2048], replicated, may hold values from 0.1 to 1.9
- expert_ids: int32 [4096, 2], P(('grp', 'sp', 'tp')), parts along dimension 0, may hold values from 0 to 15, all different within a row; in each aligned block of 128 rows (0 to 127, 128 to 255, ...) at most 32 rows name the same one
- route_weights: float32 [4096, 2], P(('grp', 'sp', 'tp')), parts along dimension 0, may hold values from 0.1 to 1
- gate_weight: bfloat16 [16, 2048, 512], P(('sp', 'tp')), may hold values from -0.125 to 0.125
- up_weight: bfloat16 [16, 2048, 512], P(('sp', 'tp')), may hold values from -0.125 to 0.125
- down_weight: bfloat16 [16, 512, 2048], P(('sp', 'tp')), may hold values from -0.5 to 0.5
Outputs:
- mixed: bfloat16 [4096, 2048], P(('grp', 'sp', 'tp')), parts along dimension 0
The draws below stay inside these ranges and needn't reach their ends.
There are 2 independent parts, one for each index of `grp`. The reference program is written for one: setup_inputs(seed, part) draws one part's arguments, and reference() takes and returns one part's arrays. A program takes and returns all parts, laid end to end along the dimension named above; an argument that names none is the same for every part. Nothing has to cross between parts.
Inputs may be any that keep to these rules, and one draw needn't show every extreme that they name: `expert_ids`: each row names 2 different experts. In the rows of one device (aligned blocks of 128 rows) no expert is named more than 32 times, and in some blocks one expert is named exactly 32 times.
All inputs are finite; a program needn't handle non-finite values.
Results may differ from the reference program's by a relative error of at most 0.014.
Values may be sent and summed in bfloat16 or wider, within the bound.
No kernel may reach another device: no remote copies, remote signals or barrier semaphores. Data moves between devices by JAX's collectives and lax.ppermute only.
A program may use at most 64 MiB of HBM per device.

```python
import math
import jax
import jax.numpy as jnp
import numpy as np
from jax import lax

D = 2048
QH = 32
KVH = 4
HEAD_SIZE = 64
WINDOW = 128
FF = 512
TOP_K = 2
TOK_DEV = 128
TOKENS = 2048
EXPERTS = 16
CAP = 32


def draw_queries(key, part):
    drawn = jnp.clip(jax.random.normal(jax.random.fold_in(key, 5), (TOKENS, QH * HEAD_SIZE), jnp.float32), -6.0, 6.0)
    return drawn.astype(jnp.bfloat16)


def draw_key_heads(key, part):
    drawn = jnp.clip(jax.random.normal(jax.random.fold_in(key, 6), (TOKENS, KVH, HEAD_SIZE), jnp.float32), -6.0, 6.0)
    return drawn.astype(jnp.bfloat16)


def steps_of(own_key, dims, pieces, least, largest):
    level, own = 1.0, jax.random.fold_in(own_key, 6)
    for position, parts in pieces:
        steps = jnp.exp(jax.random.uniform(jax.random.fold_in(own, position), (parts,), jnp.float32, least / len(pieces), largest / len(pieces)))
        level = level * jnp.repeat(steps, dims[position] // parts).reshape([-1 if axis == position else 1 for axis in range(len(dims))])
    return level


def assign_block(own_key, own, number, rows, amount, top, limit, lean):
    ranking = jax.random.permutation(own_key, amount)
    crowded, ordinary = portions_of(amount, rows * top, limit, lean, True), portions_of(amount, rows * top, limit, lean, False)
    places = jnp.arange(amount)

    def named(sizes, turn):
        used = int((sizes > 0).sum())
        fixed = max(1, used // 4)
        shifted = fixed + (places - fixed + turn * (used - fixed)) % max(1, amount - fixed)
        return jnp.zeros((amount,), jnp.int32).at[ranking[jnp.where(places < fixed, places, shifted)]].set(jnp.asarray(sizes, jnp.int32))

    sizes = jnp.where(number % 4 == 0, named(crowded, number // 4), named(ordinary, number - number // 4 - 1))
    mixed = jax.random.permutation(jax.random.fold_in(own, 3), amount)
    giver, receiver = mixed[0:amount // 2 * 2:2], mixed[1:amount // 2 * 2:2]
    room = jnp.minimum(sizes[giver] - 1, limit - sizes[receiver]) // 2
    room = jnp.where((giver == ranking[0]) | (receiver == ranking[0]) | (sizes[receiver] == 0), 0, jnp.maximum(room, 0))
    shifted = jax.random.randint(jax.random.fold_in(own, 4), (amount // 2,), 0, 1 << 20) % (room + 1)
    sizes = sizes.at[giver].add(-shifted).at[receiver].add(shifted)
    members = jnp.searchsorted(jnp.cumsum(sizes), jnp.arange(rows * top), side="right").astype(jnp.int32)
    table = members.reshape(top, rows).T
    table = table[jax.random.permutation(jax.random.fold_in(own, 1), rows)]
    turn = jax.random.randint(jax.random.fold_in(own, 2), (rows, 1), 0, top)
    return jnp.take_along_axis(table, (jnp.arange(top)[None, :] + turn) % top, axis=1)


def portions_of(amount, total, limit, skew, full):
    loads = [(1 << 20) // math.isqrt(grade ** skew) + 1 for grade in range(1, amount + 1)]
    largest = limit if full else min(limit, max(-(-total // amount), total * loads[0] // sum(loads)))
    least = 1 if total - largest >= amount - 1 else 0
    holding, rest = [largest] + [least] * (amount - 1), total - largest - least * (amount - 1)
    while rest > 0:
        free = [i for i in range(1, amount) if holding[i] < largest] or [i for i in range(1, amount) if holding[i] < limit]
        whole, left = sum([loads[i] for i in free]), rest
        for i in free:
            extra = min(limit - holding[i], max(1, left * loads[i] // whole), rest)
            holding[i] = holding[i] + extra
            rest = rest - extra
    return np.array(holding)


def normal_values(rng, dims, deviation, limit, pieces=(), kind=jnp.bfloat16):
    gain = steps_of(rng, dims, pieces, -0.22, 0.18) if pieces else 1.0
    result = jax.random.normal(rng, dims, jnp.float32) * deviation * gain
    return jnp.minimum(jnp.maximum(result, -limit), limit).astype(kind)


def setup_inputs(seed: int = 0, part: int = 0) -> dict:
    key_list = jax.random.split(jax.random.key(seed), 13)
    own_keys = jax.random.split(jax.random.fold_in(key_list[12], part), 13)
    queries = draw_queries(jax.random.fold_in(jax.random.fold_in(key_list[12], part), 71), part)
    key_heads = draw_key_heads(jax.random.fold_in(jax.random.fold_in(key_list[12], part), 71), part)
    value_heads = normal_values(own_keys[2], (TOKENS, KVH, HEAD_SIZE), 1.0, 6.0, ((0, 4), (1, 4)))
    sink_logit = jnp.clip(3.0 + 3.0 * jax.random.uniform(key_list[3], (QH,), jnp.float32) ** steps_of(key_list[3], (QH,), ((0, 4),), -0.2, 0.2), 3.0, 6.0)
    out_weight = normal_values(key_list[4], (QH * HEAD_SIZE, D), (QH * HEAD_SIZE // 32) ** -0.5, 0.75, ((0, 4),))
    residual = normal_values(own_keys[5], (TOKENS, D), 1.0, 6.0, ((0, 16),))
    norm_gain = jnp.clip(1.0 + 0.18 * jax.random.normal(key_list[6], (D,), jnp.float32), 0.1, 1.9)
    expert_ids_keys = jax.random.split(jax.random.fold_in(own_keys[7], 1), TOKENS // TOK_DEV)
    expert_ids_turns = jax.random.permutation(jax.random.fold_in(own_keys[7], 3), TOKENS // TOK_DEV)
    expert_ids = jax.vmap(lambda own, number: assign_block(jax.random.fold_in(own_keys[7], 2), own, number, TOK_DEV, EXPERTS, TOP_K, CAP, 1))(expert_ids_keys, expert_ids_turns).reshape((TOKENS, TOP_K))
    route_weights = jnp.clip(jnp.exp(math.log(1.0) - 2.3025851 * jax.random.uniform(own_keys[8], (TOKENS, TOP_K), jnp.float32) ** steps_of(own_keys[8], (TOKENS, TOP_K), ((0, 16),), -0.2, 0.2)), 0.1, 1.0)
    gate_weight = normal_values(key_list[9], (EXPERTS, D, FF), D ** -0.5, 0.125, ((0, 16),))
    up_weight = normal_values(key_list[10], (EXPERTS, D, FF), D ** -0.5, 0.125, ((0, 16),))
    down_weight = normal_values(key_list[11], (EXPERTS, FF, D), (FF // 4) ** -0.5, 0.5, ((0, 16),))
    return dict(queries=queries, key_heads=key_heads, value_heads=value_heads, sink_logit=sink_logit, out_weight=out_weight, residual=residual, norm_gain=norm_gain, expert_ids=expert_ids, route_weights=route_weights, gate_weight=gate_weight, up_weight=up_weight, down_weight=down_weight)


EPS = 1e-06

def attention(queries, key_heads, value_heads, sink_logit):
    group_size = QH // KVH
    count_of_blocks = TOKENS // WINDOW
    query_blocks = queries.reshape(count_of_blocks, WINDOW, KVH, group_size, HEAD_SIZE)
    key_blocks = key_heads.reshape(count_of_blocks, WINDOW, KVH, HEAD_SIZE)
    value_blocks = value_heads.reshape(count_of_blocks, WINDOW, KVH, HEAD_SIZE)
    blank = jnp.zeros((1, WINDOW, KVH, HEAD_SIZE), key_heads.dtype)
    key_span = jnp.concatenate([jnp.concatenate([blank, key_blocks[:-1]], 0), key_blocks], 1)
    value_span = jnp.concatenate([jnp.concatenate([blank, value_blocks[:-1]], 0), value_blocks], 1)
    query_pos = jnp.arange(WINDOW, dtype=jnp.int32)[:, None]
    key_pos = jnp.arange(2 * WINDOW, dtype=jnp.int32)[None, :]
    distance = query_pos + WINDOW - key_pos
    band = (distance >= 0) & (distance < WINDOW)
    key_start = jnp.arange(count_of_blocks, dtype=jnp.int32)[:, None] * WINDOW - WINDOW + key_pos
    allowed = band[None, :, :] & (key_start >= 0)[:, None, :]
    sinks = sink_logit.reshape(KVH, group_size)

    def one_head(packed):
        query_per_head, key_per_head, value_per_head, head_sink = packed
        logit_scores = jnp.einsum('szue,sje->suzj', query_per_head.astype(jnp.float32), key_per_head.astype(jnp.float32)) * HEAD_SIZE ** (-0.5)
        logit_scores = jnp.where(allowed[:, None], logit_scores, -jnp.inf)
        sink_col = head_sink[None, :, None, None]
        row_max = jnp.maximum(lax.optimization_barrier(jnp.max(logit_scores, axis=-1, keepdims=True)), sink_col)
        expd = jnp.exp(logit_scores - row_max)
        row_total = lax.optimization_barrier(jnp.sum(expd, axis=-1, keepdims=True)) + jnp.exp(sink_col - row_max)
        attention_probabilities = (expd / row_total).astype(jnp.bfloat16)
        return jnp.einsum('vjwu,vuo->vwjo', attention_probabilities.astype(jnp.float32), value_per_head.astype(jnp.float32)).astype(jnp.bfloat16)
    outputs = lax.map(one_head, (jnp.moveaxis(query_blocks, 2, 0), jnp.moveaxis(key_span, 2, 0), jnp.moveaxis(value_span, 2, 0), sinks))
    return jnp.moveaxis(outputs, 0, 2).reshape(TOKENS, QH * HEAD_SIZE)

def reference(queries, key_heads, value_heads, sink_logit, out_weight, residual, norm_gain, expert_ids, route_weights, gate_weight, up_weight, down_weight):
    attended = attention(queries, key_heads, value_heads, sink_logit)
    projected = jnp.dot(attended, out_weight, preferred_element_type=jnp.float32)
    stream = (residual.astype(jnp.float32) + projected).astype(jnp.bfloat16)
    wide = stream.astype(jnp.float32)
    normed = (wide * lax.rsqrt(lax.optimization_barrier(jnp.mean(wide * wide, axis=-1, keepdims=True)) + EPS) * norm_gain).astype(jnp.bfloat16)
    device_count = TOKENS // TOK_DEV
    pairs = TOK_DEV * TOP_K
    flat_ids = expert_ids.reshape(device_count, pairs)
    onehot = (flat_ids[:, :, None] == jnp.arange(EXPERTS, dtype=jnp.int32)[None, None, :]).astype(jnp.int32)
    earlier = jnp.cumsum(onehot, axis=1) - onehot
    slot_rank = lax.optimization_barrier(jnp.sum(earlier * onehot, axis=-1))
    flat_slot = (flat_ids * CAP + slot_rank).astype(jnp.int32)
    device_row = jnp.arange(device_count, dtype=jnp.int32)[:, None]
    owner_row = device_row * TOK_DEV + (jnp.arange(pairs, dtype=jnp.int32) // TOP_K)[None, :]
    shares = route_weights / lax.optimization_barrier(jnp.sum(route_weights, axis=-1, keepdims=True))
    token_in_slot = jnp.zeros((device_count, EXPERTS * CAP), jnp.int32).at[device_row, flat_slot].set(owner_row)
    slot_share = jnp.zeros((device_count, EXPERTS * CAP), jnp.float32).at[device_row, flat_slot].set(shares.reshape(device_count, pairs))

    def expert_step(summed, packed):
        w_gate_e, w_up_e, w_down_e, expert = packed
        row_index = lax.dynamic_slice_in_dim(token_in_slot, expert * CAP, CAP, 1).reshape(-1)
        row_share = lax.dynamic_slice_in_dim(slot_share, expert * CAP, CAP, 1).reshape(-1)
        rows = normed[row_index]
        gate = jnp.dot(rows, w_gate_e, preferred_element_type=jnp.float32)
        upward = jnp.dot(rows, w_up_e, preferred_element_type=jnp.float32)
        expert_hidden = (jax.nn.silu(gate) * upward).astype(jnp.bfloat16)
        expert_rows = jnp.dot(expert_hidden, w_down_e, preferred_element_type=jnp.float32).astype(jnp.bfloat16)
        summed = summed.at[row_index].add(row_share[:, None] * expert_rows.astype(jnp.float32))
        return (summed, None)
    start = jnp.zeros((TOKENS, D), jnp.float32)
    summed, _ = lax.scan(expert_step, start, (gate_weight, up_weight, down_weight, jnp.arange(EXPERTS, dtype=jnp.int32)))
    return (stream.astype(jnp.float32) + summed).astype(jnp.bfloat16)
```

```python
import jax
import jax.numpy as jnp
from jax import lax
from jax.sharding import PartitionSpec as P

WINDOW = 128


EPS = 1e-06
CHUNKS = 2
DIRECT_LIMIT = 4


def from_behind(value, axis, steps):
    count = lax.axis_size(axis)
    initial, last = (max(0, -steps), min(count, count - steps))
    return lax.ppermute(value, axis, [(source, source + steps) for source in range(initial, last)])


def exchange(value, across_sp, across_tp):
    if across_sp == 0 and across_tp == 0:
        return value
    sp_count = lax.axis_size("sp")
    tp_count = lax.axis_size("tp")
    pairs = [
        (s * tp_count + t, (s ^ across_sp) * tp_count + (t ^ across_tp))
        for s in range(sp_count)
        for t in range(tp_count)
    ]
    return lax.ppermute(value, ("sp", "tp"), pairs)


def swap(boxes, offsets, direct):
    if direct:
        return [exchange(boxes[n], a, b) for n, (a, b) in enumerate(offsets)]
    stacked = jnp.stack([boxes[n] for n in range(len(offsets))])
    stacked = stacked.reshape(len(offsets) // 2, 2, *stacked.shape[1:])
    moved = lax.all_to_all(stacked, "sp", split_axis=0, concat_axis=0, tiled=True)
    moved = jnp.stack([moved[:, 0], exchange(moved[:, 1], 0, 1)], 1)
    return list(moved.reshape(len(offsets), *moved.shape[2:]))


def on_device(
    queries,
    key_heads,
    value_heads,
    sink_logit,
    out_weight,
    residual,
    norm_gain,
    expert_ids,
    route_weights,
    gate_weight,
    up_weight,
    down_weight,
):
    rows_sp = queries.shape[0]
    kv_local = key_heads.shape[1]
    head_dim = key_heads.shape[2]
    heads_local = queries.shape[1] // head_dim
    group_size = heads_local // kv_local
    window = WINDOW
    count_of_blocks = rows_sp // window
    edge = jnp.stack([key_heads[rows_sp - window :], value_heads[rows_sp - window :]])
    tail_rows = from_behind(edge, "sp", 1)
    key_blocks = jnp.concatenate([tail_rows[0], key_heads], 0).reshape(
        count_of_blocks + 1, window, kv_local, head_dim
    )
    value_blocks = jnp.concatenate([tail_rows[1], value_heads], 0).reshape(
        count_of_blocks + 1, window, kv_local, head_dim
    )
    key_span = jnp.concatenate([key_blocks[:-1], key_blocks[1:]], 1)
    value_span = jnp.concatenate([value_blocks[:-1], value_blocks[1:]], 1)
    query_pos = jnp.arange(window, dtype=jnp.int32)[:, None]
    key_pos = jnp.arange(2 * window, dtype=jnp.int32)[None, :]
    distance = query_pos + window - key_pos
    band = (distance >= 0) & (distance < window)
    key_start = (
        lax.axis_index("sp") * rows_sp
        + jnp.arange(count_of_blocks, dtype=jnp.int32)[:, None] * window
        - window
        + key_pos
    )
    allowed = band[None, :, :] & (key_start >= 0)[:, None, :]
    query_blocks = queries.reshape(count_of_blocks, window, kv_local, group_size, head_dim)
    logit_scores = jnp.einsum(
        "bqhgd,bkhd->bhgqk", query_blocks, key_span, preferred_element_type=jnp.float32
    ) * head_dim ** (-0.5)
    logit_scores = jnp.where(allowed[:, None, None], logit_scores, -jnp.inf)
    sink_col = sink_logit.reshape(kv_local, group_size)[None, :, :, None, None]
    row_max = jnp.maximum(jnp.max(logit_scores, axis=-1, keepdims=True), sink_col)
    expd = jnp.exp(logit_scores - row_max)
    row_total = jnp.sum(expd, axis=-1, keepdims=True) + jnp.exp(sink_col - row_max)
    attention_probabilities = (expd / row_total).astype(jnp.bfloat16)
    attended = jnp.einsum(
        "bhgqk,bkhd->bqhgd", attention_probabilities, value_span, preferred_element_type=jnp.float32
    ).astype(jnp.bfloat16)
    attended = attended.reshape(rows_sp, heads_local * head_dim)
    rows_dev = residual.shape[0]
    width = residual.shape[1]
    sp_count = lax.axis_size("sp")
    tp_count = lax.axis_size("tp")
    experts_total = sp_count * tp_count
    top_k = expert_ids.shape[1]
    capacity = max(2, 2 * top_k * rows_dev // experts_total)
    peers = tp_count // 2
    chunks = CHUNKS
    cols = width // chunks
    place_sp = lax.axis_index("sp")
    place_tp = lax.axis_index("tp")
    parity = place_tp % 2
    column = place_tp // 2

    out_weight_twin = exchange(out_weight, 0, 1)
    residual_all = jnp.stack([exchange(residual, 0, 2 * m) for m in range(peers)])
    ids_all = jnp.stack([exchange(expert_ids, 0, 2 * m) for m in range(peers)])
    weights_all = jnp.stack([exchange(route_weights, 0, 2 * m) for m in range(peers)])
    shares = weights_all / jnp.sum(weights_all, axis=-1, keepdims=True)

    offsets = [(a, b) for a in range(sp_count) for b in range(2)]
    direct = sp_count <= DIRECT_LIMIT
    owners = jnp.stack(
        [
            (place_sp ^ a if direct else a) * tp_count + column * 2 + (parity ^ b)
            for a, b in offsets
        ]
    )
    matches = ids_all[:, None, :, :] == owners[None, :, None, None]
    hit = jnp.any(matches, axis=-1)
    token_share = jnp.sum(jnp.where(matches, shares[:, None], 0.0), axis=-1)
    before = jnp.triu(jnp.ones((rows_dev, rows_dev), jnp.bfloat16), 1)
    rank = jnp.dot(hit.astype(jnp.bfloat16), before, preferred_element_type=jnp.float32)
    slots = jnp.arange(capacity, dtype=jnp.int32)
    chosen = hit[:, :, None, :] & (rank.astype(jnp.int32)[:, :, None, :] == slots[None, None, :, None])
    same = (jnp.arange(peers)[:, None] == jnp.arange(peers)[None, :])
    spread = chosen.transpose(1, 0, 2, 3)[:, :, :, None, :] & same[None, :, None, :, None]
    pick = spread.reshape(len(offsets), peers * capacity, peers * rows_dev).astype(jnp.bfloat16)
    scaled = jnp.where(
        spread, token_share.transpose(1, 0, 2)[:, None, None], 0.0
    ).reshape(len(offsets) * peers * capacity, peers * rows_dev)
    scaled_high = scaled.astype(jnp.bfloat16)
    scaled_low = (scaled - scaled_high.astype(jnp.float32)).astype(jnp.bfloat16)

    blocks = attended.reshape(peers, 2, rows_dev, -1)
    by_peer = jnp.stack([blocks[column ^ m] for m in range(peers)])
    kept = jnp.take(by_peer, parity, axis=1).reshape(peers * rows_dev, -1)
    given = jnp.take(by_peer, 1 - parity, axis=1).reshape(peers * rows_dev, -1)
    taken = exchange(given, 0, 1)

    stream_parts = []
    gate = 0.0
    upward = 0.0
    squares = 0.0
    for j in range(chunks):
        span = slice(j * cols, (j + 1) * cols)
        partial = jnp.dot(
            kept, out_weight[:, span], preferred_element_type=jnp.float32
        ) + jnp.dot(taken, out_weight_twin[:, span], preferred_element_type=jnp.float32)
        partial = partial.reshape(peers, rows_dev, cols)
        shared = partial.astype(jnp.bfloat16)
        total = residual_all[:, :, span].astype(jnp.float32) + partial
        for m in range(1, peers):
            heard = exchange(shared, 0, 2 * m)
            total = total + jnp.stack([heard[i ^ m] for i in range(peers)]).astype(jnp.float32)
        stream = total.astype(jnp.bfloat16)
        stream_parts.append(stream[0])
        sources = stream.reshape(peers * rows_dev, cols)
        boxes = [
            jnp.dot(pick[n], sources, preferred_element_type=jnp.float32).astype(jnp.bfloat16)
            for n in range(len(offsets))
        ]
        rows = jnp.concatenate(swap(boxes, offsets, direct), 0).astype(jnp.float32)
        squares = squares + jnp.sum(rows * rows, axis=-1, keepdims=True)
        rows = (rows * norm_gain[span]).astype(jnp.bfloat16)
        gate = gate + jnp.dot(rows, gate_weight[0, span], preferred_element_type=jnp.float32)
        upward = upward + jnp.dot(rows, up_weight[0, span], preferred_element_type=jnp.float32)
    scale = lax.rsqrt(squares / width + EPS)
    expert_hidden = (jax.nn.silu(gate * scale) * (upward * scale)).astype(jnp.bfloat16)
    mixed = []
    for j in range(chunks):
        span = slice(j * cols, (j + 1) * cols)
        results = jnp.dot(
            expert_hidden, down_weight[0, :, span], preferred_element_type=jnp.float32
        ).astype(jnp.bfloat16).reshape(len(offsets), peers * capacity, cols)
        returned = jnp.concatenate(swap(results, offsets, direct), 0)
        summed = lax.dot_general(
            scaled_high, returned, (((0,), (0,)), ((), ())), preferred_element_type=jnp.float32
        ) + lax.dot_general(
            scaled_low, returned, (((0,), (0,)), ((), ())), preferred_element_type=jnp.float32
        )
        summed = summed.reshape(peers, rows_dev, cols)
        total = stream_parts[j].astype(jnp.float32) + summed[0]
        for m in range(1, peers):
            total = total + exchange(summed[m].astype(jnp.bfloat16), 0, 2 * m).astype(jnp.float32)
        mixed.append(total.astype(jnp.bfloat16))
    return jnp.concatenate(mixed, 1)


def solution(mesh):
    return jax.shard_map(
        on_device,
        mesh=mesh,
        in_specs=(
            P(("grp", "sp"), "tp"),
            P(("grp", "sp"), "tp", None),
            P(("grp", "sp"), "tp", None),
            P("tp"),
            P("tp", None),
            P(("grp", "sp", "tp"), None),
            P(),
            P(("grp", "sp", "tp"), None),
            P(("grp", "sp", "tp"), None),
            P(("sp", "tp"), None, None),
            P(("sp", "tp"), None, None),
            P(("sp", "tp"), None, None),
        ),
        out_specs=P(("grp", "sp", "tp"), None),
        check_vma=False,
    )
```

```python
import jax
import jax.numpy as jnp
from jax import lax
from jax.sharding import PartitionSpec as P

WINDOW = 128


EPS = 1e-06
OUTBOUND = (3, 5)
INBOUND = (5, 3)
DIRECT_LIMIT = 4


def from_behind(value, axis, steps):
    count = lax.axis_size(axis)
    initial, last = (max(0, -steps), min(count, count - steps))
    return lax.ppermute(value, axis, [(source, source + steps) for source in range(initial, last)])


def spans_of(width, parts):
    unit = width // sum(parts)
    edges = [unit * sum(parts[:i]) for i in range(len(parts))] + [width]
    return [slice(low, high) for low, high in zip(edges[:-1], edges[1:])]


def exchange(value, across_sp, across_tp):
    if across_sp == 0 and across_tp == 0:
        return value
    sp_count = lax.axis_size("sp")
    tp_count = lax.axis_size("tp")
    pairs = [
        (s * tp_count + t, (s ^ across_sp) * tp_count + (t ^ across_tp))
        for s in range(sp_count)
        for t in range(tp_count)
    ]
    return lax.ppermute(value, ("sp", "tp"), pairs)


def swap(boxes, offsets, direct):
    if direct:
        return [exchange(boxes[n], a, b) for n, (a, b) in enumerate(offsets)]
    stacked = jnp.stack([boxes[n] for n in range(len(offsets))])
    stacked = stacked.reshape(len(offsets) // 2, 2, *stacked.shape[1:])
    moved = lax.all_to_all(stacked, "sp", split_axis=0, concat_axis=0, tiled=True)
    moved = jnp.stack([moved[:, 0], exchange(moved[:, 1], 0, 1)], 1)
    return list(moved.reshape(len(offsets), *moved.shape[2:]))


def on_device(
    queries,
    key_heads,
    value_heads,
    sink_logit,
    out_weight,
    residual,
    norm_gain,
    expert_ids,
    route_weights,
    gate_weight,
    up_weight,
    down_weight,
):
    rows_sp = queries.shape[0]
    kv_local = key_heads.shape[1]
    head_dim = key_heads.shape[2]
    heads_local = queries.shape[1] // head_dim
    group_size = heads_local // kv_local
    window = WINDOW
    count_of_blocks = rows_sp // window
    edge = jnp.stack([key_heads[rows_sp - window :], value_heads[rows_sp - window :]])
    tail_rows = from_behind(edge, "sp", 1)
    key_blocks = jnp.concatenate([tail_rows[0], key_heads], 0).reshape(
        count_of_blocks + 1, window, kv_local, head_dim
    )
    value_blocks = jnp.concatenate([tail_rows[1], value_heads], 0).reshape(
        count_of_blocks + 1, window, kv_local, head_dim
    )
    key_span = jnp.concatenate([key_blocks[:-1], key_blocks[1:]], 1)
    value_span = jnp.concatenate([value_blocks[:-1], value_blocks[1:]], 1)
    query_pos = jnp.arange(window, dtype=jnp.int32)[:, None]
    key_pos = jnp.arange(2 * window, dtype=jnp.int32)[None, :]
    distance = query_pos + window - key_pos
    band = (distance >= 0) & (distance < window)
    key_start = (
        lax.axis_index("sp") * rows_sp
        + jnp.arange(count_of_blocks, dtype=jnp.int32)[:, None] * window
        - window
        + key_pos
    )
    allowed = band[None, :, :] & (key_start >= 0)[:, None, :]
    query_blocks = queries.reshape(count_of_blocks, window, kv_local, group_size, head_dim)
    logit_scores = jnp.einsum(
        "bqhgd,bkhd->bhgqk", query_blocks, key_span, preferred_element_type=jnp.float32
    ) * head_dim ** (-0.5)
    logit_scores = jnp.where(allowed[:, None, None], logit_scores, -jnp.inf)
    sink_col = sink_logit.reshape(kv_local, group_size)[None, :, :, None, None]
    row_max = jnp.maximum(jnp.max(logit_scores, axis=-1, keepdims=True), sink_col)
    expd = jnp.exp(logit_scores - row_max)
    row_total = jnp.sum(expd, axis=-1, keepdims=True) + jnp.exp(sink_col - row_max)
    attention_probabilities = (expd / row_total).astype(jnp.bfloat16)
    attended = jnp.einsum(
        "bhgqk,bkhd->bqhgd", attention_probabilities, value_span, preferred_element_type=jnp.float32
    ).astype(jnp.bfloat16)
    attended = attended.reshape(rows_sp, heads_local * head_dim)
    rows_dev = residual.shape[0]
    width = residual.shape[1]
    sp_count = lax.axis_size("sp")
    tp_count = lax.axis_size("tp")
    experts_total = sp_count * tp_count
    top_k = expert_ids.shape[1]
    capacity = max(2, 2 * top_k * rows_dev // experts_total)
    peers = tp_count // 2
    place_sp = lax.axis_index("sp")
    place_tp = lax.axis_index("tp")
    parity = place_tp % 2
    column = place_tp // 2

    out_weight_twin = exchange(out_weight, 0, 1)
    ids_all = jnp.stack([exchange(expert_ids, 0, 2 * m) for m in range(peers)])
    weights_all = jnp.stack([exchange(route_weights, 0, 2 * m) for m in range(peers)])
    shares = weights_all / jnp.sum(weights_all, axis=-1, keepdims=True)

    direct = sp_count <= DIRECT_LIMIT
    order = reversed(range(sp_count)) if direct else range(sp_count)
    offsets = [(a, b) for a in order for b in range(2)]
    owners = jnp.stack(
        [
            (place_sp ^ a if direct else a) * tp_count + column * 2 + (parity ^ b)
            for a, b in offsets
        ]
    )
    matches = ids_all[:, None, :, :] == owners[None, :, None, None]
    hit = jnp.any(matches, axis=-1)
    token_share = jnp.sum(jnp.where(matches, shares[:, None], 0.0), axis=-1)
    before = jnp.triu(jnp.ones((rows_dev, rows_dev), jnp.bfloat16), 1)
    rank = jnp.dot(hit.astype(jnp.bfloat16), before, preferred_element_type=jnp.float32)
    slots = jnp.arange(capacity, dtype=jnp.int32)
    chosen = hit[:, :, None, :] & (rank.astype(jnp.int32)[:, :, None, :] == slots[None, None, :, None])
    same = (jnp.arange(peers)[:, None] == jnp.arange(peers)[None, :])
    spread = chosen.transpose(1, 0, 2, 3)[:, :, :, None, :] & same[None, :, None, :, None]
    pick = spread.reshape(len(offsets), peers * capacity, peers * rows_dev).astype(jnp.bfloat16)
    scaled = jnp.where(
        spread, token_share.transpose(1, 0, 2)[:, None, None], 0.0
    ).reshape(len(offsets) * peers * capacity, peers * rows_dev)
    scaled_high = scaled.astype(jnp.bfloat16)
    scaled_low = (scaled - scaled_high.astype(jnp.float32)).astype(jnp.bfloat16)

    blocks = attended.reshape(peers, 2, rows_dev, -1)
    by_peer = jnp.stack([blocks[column ^ m] for m in range(peers)])
    kept = jnp.take(by_peer, parity, axis=1).reshape(peers * rows_dev, -1)
    given = jnp.take(by_peer, 1 - parity, axis=1).reshape(peers * rows_dev, -1)
    taken = exchange(given, 0, 1)

    partials = []
    for span in spans_of(width, OUTBOUND):
        partial = jnp.dot(
            kept, out_weight[:, span], preferred_element_type=jnp.float32
        ) + jnp.dot(taken, out_weight_twin[:, span], preferred_element_type=jnp.float32)
        partial = partial.reshape(peers, rows_dev, -1)
        own = partial[0] + residual[:, span].astype(jnp.float32)
        partials.append([own] + [partial[m] for m in range(1, peers)])
    shared = [jnp.stack(p).astype(jnp.bfloat16) for p in partials]

    stream_parts = []
    sent = []
    landed = []
    gate = 0.0
    upward = 0.0
    squares = 0.0
    for j, span in enumerate(spans_of(width, OUTBOUND)):
        total = list(partials[j])
        for m in range(1, peers):
            heard = exchange(shared[j], 0, 2 * m)
            total = [total[i] + heard[i ^ m].astype(jnp.float32) for i in range(peers)]
        stream = lax.optimization_barrier(jnp.stack(total).astype(jnp.bfloat16))
        stream_parts.append(stream[0])
        sources = stream.reshape(peers * rows_dev, -1)
        boxes = [
            jnp.dot(pick[n], sources, preferred_element_type=jnp.float32).astype(jnp.bfloat16)
            for n in range(len(offsets))
        ]
        sent.append(boxes)
        landed.append(swap(boxes, offsets, direct))
    for j, span in enumerate(spans_of(width, OUTBOUND)):
        if j + 1 < len(landed):
            landed[j], sent[j + 1] = lax.optimization_barrier((landed[j], sent[j + 1]))
        rows = jnp.concatenate(landed[j], 0).astype(jnp.float32)
        squares = squares + jnp.sum(rows * rows, axis=-1, keepdims=True)
        rows = (rows * norm_gain[span]).astype(jnp.bfloat16)
        gate = gate + jnp.dot(rows, gate_weight[0, span], preferred_element_type=jnp.float32)
        upward = upward + jnp.dot(rows, up_weight[0, span], preferred_element_type=jnp.float32)
    scale = lax.rsqrt(squares / width + EPS)
    expert_hidden = (jax.nn.silu(gate * scale) * (upward * scale)).astype(jnp.bfloat16)
    stream_own = jnp.concatenate(stream_parts, 1)
    returns = []
    leaving_rows = []
    for span in spans_of(width, INBOUND):
        results = jnp.dot(
            expert_hidden, down_weight[0, :, span], preferred_element_type=jnp.float32
        ).astype(jnp.bfloat16).reshape(len(offsets), peers * capacity, -1)
        leaving_rows.append(results)
        returns.append(swap(results, offsets, direct))
    mixed = []
    leaving = None
    for j, span in enumerate(spans_of(width, INBOUND)):
        if leaving is not None:
            returns[j], leaving = lax.optimization_barrier((returns[j], leaving))
        if j + 1 < len(returns):
            returns[j], leaving_rows[j + 1] = lax.optimization_barrier(
                (returns[j], leaving_rows[j + 1])
            )
        returned = jnp.concatenate(returns[j], 0)
        summed = lax.dot_general(
            scaled_high, returned, (((0,), (0,)), ((), ())), preferred_element_type=jnp.float32
        ) + lax.dot_general(
            scaled_low, returned, (((0,), (0,)), ((), ())), preferred_element_type=jnp.float32
        )
        summed = summed.reshape(peers, rows_dev, -1)
        total = stream_own[:, span].astype(jnp.float32) + summed[0]
        leaving = [summed[m].astype(jnp.bfloat16) for m in range(1, peers)]
        for m in range(1, peers):
            total = total + exchange(leaving[m - 1], 0, 2 * m).astype(jnp.float32)
        mixed.append(total.astype(jnp.bfloat16))
    return jnp.concatenate(mixed, 1)


def solution(mesh):
    return jax.shard_map(
        on_device,
        mesh=mesh,
        in_specs=(
            P(("grp", "sp"), "tp"),
            P(("grp", "sp"), "tp", None),
            P(("grp", "sp"), "tp", None),
            P("tp"),
            P("tp", None),
            P(("grp", "sp", "tp"), None),
            P(),
            P(("grp", "sp", "tp"), None),
            P(("grp", "sp", "tp"), None),
            P(("sp", "tp"), None, None),
            P(("sp", "tp"), None, None),
            P(("sp", "tp"), None, None),
        ),
        out_specs=P(("grp", "sp", "tp"), None),
        check_vma=False,
    )
```
